256 devices in a mesh: sp: 32 (over z, x), tp: 8 (over y, core).
Axes of the slice: x: 4, y: 4, z: 8, core: 2. Of those that a mesh axis runs over, the one named last changes fastest.
Arguments:
- inputs: bfloat16 [12288, 4096], P('sp', 'tp'), may hold values from -40 to 40, as said below
- query_weight: bfloat16 [2, 4096, 1024], P(None, None, 'tp'), may hold values from -0.2 to 0.2
- key_weight: bfloat16 [2, 4096, 1024], P(None, None, 'tp'), may hold values from -0.2 to 0.2
- value_weight: bfloat16 [4096, 2048], P(None, 'tp'), may hold values from -0.09375 to 0.09375
- pool_weight: bfloat16 [4096, 2048], P(None, 'tp'), may hold values from -0.09375 to 0.09375
- mix_lambda: float32 [16], P('tp'), may hold values from 0.3 to 0.8
- head_gain: float32 [128], replicated, may hold values from 0.1 to 1.9
- attn_out_weight: bfloat16 [2048, 4096], P('tp'), may hold values from -0.125 to 0.125
- pool_out_weight: bfloat16 [2048, 4096], P('tp'), may hold values from -0.125 to 0.125
Outputs:
- mixed: bfloat16 [12288, 4096], P(('sp', 'tp'))
- log_totals: float32 [2, 16, 12288], P(None, 'tp', 'sp')
The draws below stay inside these ranges and needn't reach their ends.
Inputs may be any that keep to these rules, and one draw needn't show every extreme that they name: inputs of order one, in some draws a few rows larger.
All inputs are finite; a program needn't handle non-finite values.
Results may differ from the reference program's by a relative error of at most 0.015.
Values may be sent and summed in bfloat16 or wider, within the bound.
A program may use at most 192 MiB of HBM per device.

```python
import jax
import jax.numpy as jnp
from jax import lax

D = 4096
HEADS = 16
HEAD_DIM = 64
POOL_WIDTH = 2048
TOK_DEV = 384
TOKENS = 12288
N_TP = 8


def shared_query(key):
    return jax.random.normal(jax.random.fold_in(key, 101), (2, D, HEADS * HEAD_DIM), jnp.float32) * (1.32 * D ** (-0.5))


def draw_query_weight(key, part):
    return jnp.clip(shared_query(key), -0.199, 0.199).astype(jnp.bfloat16)


def draw_key_weight(key, part):
    own = jax.random.normal(jax.random.fold_in(key, 202), (2, D, HEADS * HEAD_DIM), jnp.float32) * (1.32 * D ** (-0.5))
    return jnp.clip(own, -0.199, 0.199).astype(jnp.bfloat16)


def draw_inputs(key, part):
    base = jnp.clip(jax.random.normal(jax.random.fold_in(key, 303), (TOKENS, D), jnp.float32), -6.0, 6.0)
    return jnp.clip(base, -40.0, 40.0).astype(jnp.bfloat16)


def level_of(key, shape, cuts, smallest, high):
    level, own = 1.0, jax.random.fold_in(key, 6)
    for axis_at, shards_of in cuts:
        heights = jnp.exp(jax.random.uniform(jax.random.fold_in(own, axis_at), (shards_of,), jnp.float32, smallest / len(cuts), high / len(cuts)))
        level = level * jnp.repeat(heights, shape[axis_at] // shards_of).reshape([-1 if axis == axis_at else 1 for axis in range(len(shape))])
    return level


def bell_draw(rng, extent, deviation, most, shards=(), kind=jnp.bfloat16):
    array = jax.random.normal(rng, extent, jnp.float32) * deviation
    if len(shards) > 0:
        array = level_of(rng, extent, shards, -0.22, 0.18) * array
    return jnp.clip(array, min=-most, max=most).astype(kind)


def setup_inputs(seed: int = 0) -> dict:
    seeds = jax.random.split(jax.random.key(seed), 10)
    inputs = draw_inputs(jax.random.fold_in(seeds[9], 71), 0)
    query_weight = draw_query_weight(jax.random.fold_in(seeds[9], 71), 0)
    key_weight = draw_key_weight(jax.random.fold_in(seeds[9], 71), 0)
    value_weight = bell_draw(seeds[3], (D, HEADS * 2 * HEAD_DIM), D ** -0.5, 0.09375, ((1, 8),))
    pool_weight = bell_draw(seeds[4], (D, POOL_WIDTH), D ** -0.5, 0.09375, ((1, 8),))
    mix_lambda = jnp.clip(0.3 + 0.5 * jax.random.uniform(seeds[5], (HEADS,), jnp.float32) ** level_of(seeds[5], (HEADS,), ((0, 8),), -0.2, 0.2), 0.3, 0.8)
    head_gain = jnp.clip(1.0 + 0.18 * jax.random.normal(seeds[6], (2 * HEAD_DIM,), jnp.float32), 0.1, 1.9)
    attn_out_weight = bell_draw(seeds[7], (HEADS * 2 * HEAD_DIM, D), (HEADS * 2 * HEAD_DIM) ** -0.5, 0.125, ((0, 8),))
    pool_out_weight = bell_draw(seeds[8], (POOL_WIDTH, D), POOL_WIDTH ** -0.5, 0.125, ((0, 8),))
    return dict(inputs=inputs, query_weight=query_weight, key_weight=key_weight, value_weight=value_weight, pool_weight=pool_weight, mix_lambda=mix_lambda, head_gain=head_gain, attn_out_weight=attn_out_weight, pool_out_weight=pool_out_weight)


def head_block(query_rows, key_rows, value_rows, lam_value, head_gain):
    scores = jnp.einsum('mqd,mkd->mqk', query_rows.astype(jnp.float32), key_rows.astype(jnp.float32)) * HEAD_DIM ** (-0.5)
    row_max = lax.optimization_barrier(jnp.max(scores, axis=-1))
    expo = jnp.exp(scores - row_max[..., None])
    totals = lax.optimization_barrier(jnp.sum(expo, axis=-1))
    weights = expo.astype(jnp.bfloat16).astype(jnp.float32)
    numer = jnp.einsum('mqk,ke->mqe', weights, value_rows.astype(jnp.float32))
    diff = numer[0] / totals[0][:, None] - lam_value * numer[1] / totals[1][:, None]
    scaled = diff * lax.rsqrt(lax.optimization_barrier(jnp.mean(diff * diff, axis=-1, keepdims=True)) + 1e-05) * head_gain
    return (scaled.astype(jnp.bfloat16), row_max + jnp.log(totals))

def reference(inputs, query_weight, key_weight, value_weight, pool_weight, mix_lambda, head_gain, attn_out_weight, pool_out_weight):
    total_tok = inputs.shape[0]
    queries = jnp.stack([jnp.dot(inputs, query_weight[m], preferred_element_type=jnp.float32) for m in range(2)]).astype(jnp.bfloat16)
    keys = jnp.stack([jnp.dot(inputs, key_weight[m], preferred_element_type=jnp.float32) for m in range(2)]).astype(jnp.bfloat16)
    values = jnp.dot(inputs, value_weight, preferred_element_type=jnp.float32).astype(jnp.bfloat16)
    pool_in = jnp.dot(inputs, pool_weight, preferred_element_type=jnp.float32).astype(jnp.bfloat16)
    query_heads = queries.reshape(2, total_tok, HEADS, HEAD_DIM).transpose(2, 0, 1, 3)
    key_heads = keys.reshape(2, total_tok, HEADS, HEAD_DIM).transpose(2, 0, 1, 3)
    value_heads = values.reshape(total_tok, HEADS, 2 * HEAD_DIM).transpose(1, 0, 2)
    blocks = total_tok // TOK_DEV

    def one_head(packed):
        query_rows, key_rows, value_rows, lam_value = packed
        query_blocks = query_rows.reshape(2, blocks, TOK_DEV, HEAD_DIM).transpose(1, 0, 2, 3)
        outs, logs = lax.map(lambda block: head_block(block, key_rows, value_rows, lam_value, head_gain), query_blocks)
        return (outs.reshape(total_tok, 2 * HEAD_DIM), logs.transpose(1, 0, 2).reshape(2, total_tok))
    head_outs, head_logs = lax.map(one_head, (query_heads, key_heads, value_heads, mix_lambda))
    attn = head_outs.transpose(1, 0, 2).reshape(total_tok, HEADS * 2 * HEAD_DIM)
    log_totals = head_logs.transpose(1, 0, 2)
    pool_f = pool_in.astype(jnp.float32)
    padded = jnp.pad(pool_f, ((8, 8), (0, 0)))
    position = jnp.arange(total_tok, dtype=jnp.int32)
    group_width = POOL_WIDTH // 4
    pieces = []
    for group_index, reach in enumerate((2, 4, 8, 16)):
        radius = reach // 2
        cols = slice(group_index * group_width, (group_index + 1) * group_width)
        window_sum = padded[8 - radius:8 - radius + total_tok, cols]
        for shift_by in range(-radius + 1, radius):
            window_sum = window_sum + padded[8 + shift_by:8 + shift_by + total_tok, cols]
        low = jnp.clip(position - radius, 0, total_tok)
        high = jnp.clip(position + radius, 0, total_tok)
        pieces.append(window_sum / (high - low).astype(jnp.float32)[:, None] - pool_f[:, cols])
    pooled = jnp.concatenate(pieces, axis=1).astype(jnp.bfloat16)
    attn_cols = HEADS * 2 * HEAD_DIM // N_TP
    pool_cols = POOL_WIDTH // N_TP
    summed = jnp.zeros((total_tok, D), jnp.float32)
    for group_index in range(N_TP):
        a_cols = slice(group_index * attn_cols, (group_index + 1) * attn_cols)
        p_cols = slice(group_index * pool_cols, (group_index + 1) * pool_cols)
        partial_value = jnp.dot(attn[:, a_cols], attn_out_weight[a_cols], preferred_element_type=jnp.float32)
        partial_value = partial_value + jnp.dot(pooled[:, p_cols], pool_out_weight[p_cols], preferred_element_type=jnp.float32)
        rounded = lax.optimization_barrier(partial_value.astype(jnp.bfloat16))
        summed = summed + rounded.astype(jnp.float32)
    return (summed.astype(jnp.bfloat16), log_totals)
```

```python
import functools
import math

import jax
import jax.numpy as jnp
from jax import lax
from jax.experimental import pallas as pl
from jax.experimental.pallas import tpu as pltpu
from jax.sharding import PartitionSpec as P

MESH = pl.DeviceIdType.MESH
F32 = jnp.float32
BF16 = jnp.bfloat16

NX, NY, NZ = 4, 4, 8
TOK = 384
CH = 128
NT = TOK // CH
D = 4096
FEAT = 512
HD = 64
SCALE = HD**-0.5 * math.log2(math.e)
LN2 = math.log(2.0)
TILE = 256
COLS = 2 * 2 * TOK
KEYS = 2 * TOK
PAD = 16
OUT = 48
NB = 512


def kernel(
    lam_ref, gain_ref, x_hbm, qw, kw, vw, pw, ow, pow_,
    mixed_ref, logt_ref,
    xg, wts, wo, sbuf, sq, kv, qin, qt2, acc, mrow, lrow, lamb,
    pbuf, pf, ps, pooled, pin, psib, ob, at_in, lgs, lg_in,
    amat, own, keep, via_s, via_r, raw_s, sum_s, fin, sc, mx, rs, wt,
    xsem, wsem, ysend, yrecv, a2s, a2r, rsend, rrecv, ssend, srecv,
    wos, wor, lms, lmr, hs, hr, pxs, pxr, bs, br, ls, lr, vs, vr, fs, fr,
):
    me_sp = lax.axis_index("sp")
    me_tp = lax.axis_index("tp")
    z, x = lax.div(me_sp, NX), lax.rem(me_sp, NX)
    y, c = lax.div(me_tp, 2), lax.rem(me_tp, 2)
    d = 1 - 2 * c
    sib = (me_sp, y * 2 + 1 - c)
    y_next, y_prev = lax.rem(y + d + NY, NY), lax.rem(y - d + NY, NY)
    y_opp = lax.rem(y + 2, NY)
    z_next = lax.rem(z + d + NZ, NZ)
    ring_next = (z_next * NX + x, me_tp)
    x_core = lax.div(x, 2)
    x_pos = lax.rem(x, 2)

    def remote(src, dst, send, recv, device):
        return pltpu.make_async_remote_copy(
            src_ref=src, dst_ref=dst, send_sem=send, recv_sem=recv,
            device_id=device, device_id_type=MESH,
        )

    def cols_of(tp):
        return pl.ds(pl.multiple_of(tp * FEAT, FEAT), FEAT)

    barrier = pltpu.get_barrier_semaphore()
    partners = [sib]
    for step in range(1, NX):
        for core in range(2):
            partners.append((z * NX + lax.rem(x + step, NX), y * 2 + core))
    partners += [(me_sp, lax.rem(y + 1, NY) * 2 + c), (me_sp, lax.rem(y + NY - 1, NY) * 2 + c)]
    partners += [(lax.rem(z + 1, NZ) * NX + x, me_tp), (lax.rem(z + NZ - 1, NZ) * NX + x, me_tp)]
    partners += [
        (lax.rem(me_sp + 1, NX * NZ), me_tp),
        (lax.rem(me_sp + NX * NZ - 1, NX * NZ), me_tp),
    ]
    pbuf[0:PAD] = jnp.zeros((PAD, 256), BF16)
    pbuf[PAD + TOK :] = jnp.zeros((PAD, 256), BF16)
    for partner in partners:
        pl.semaphore_signal(barrier, inc=1, device_id=partner, device_id_type=MESH)

    x_copies = [
        pltpu.make_async_copy(
            x_hbm.at[pl.ds(t * CH, CH), :], xg.at[t, :, cols_of(me_tp)], xsem.at[t]
        )
        for t in range(NT)
    ]
    w_copies = [
        pltpu.make_async_copy(src, dst, wsem.at[i // 6])
        for i, (src, dst) in enumerate(
            [
                (kw.at[0], wts.at[:, pl.ds(0, 128)]),
                (kw.at[1], wts.at[:, pl.ds(128, 128)]),
                (vw, wts.at[:, pl.ds(256, 256)]),
                (qw.at[0], wts.at[:, pl.ds(512, 128)]),
                (qw.at[1], wts.at[:, pl.ds(640, 128)]),
                (pw, wts.at[:, pl.ds(768, 256)]),
                (ow, wo.at[c, 0]),
                (pow_, wo.at[c, 1]),
            ]
        )
    ]
    for copy in x_copies:
        copy.start()
    for copy in w_copies:
        copy.start()

    lane = lax.broadcasted_iota(jnp.int32, (8, 128), 1)
    lamb[c] = jnp.where(lane == 0, lam_ref[0], lam_ref[1])
    acc[...] = jnp.zeros_like(acc)
    lrow[...] = jnp.zeros_like(lrow)
    mrow[...] = jnp.full(mrow.shape, -1e30, F32)

    pl.semaphore_wait(barrier, len(partners))

    def ycopy(t, kind, tp, device):
        region = xg.at[t, :, cols_of(tp)]
        return remote(region, region, ysend.at[0], yrecv.at[t, min(kind, 3)], device)

    next_dev, prev_dev = (me_sp, y_next * 2 + c), (me_sp, y_prev * 2 + c)
    tp_prev, tp_next, tp_opp = y_prev * 2 + c, y_next * 2 + c, y_opp * 2 + c
    mine = [
        (0, me_tp, next_dev), (1, me_tp, prev_dev), (2, tp_prev, next_dev),
        (3, me_tp, sib), (4, tp_prev, sib), (5, tp_next, sib), (6, tp_opp, sib),
    ]
    arriving = [
        tp_prev, tp_next, tp_opp,
        y * 2 + 1 - c, y_next * 2 + 1 - c, y_prev * 2 + 1 - c, y_opp * 2 + 1 - c,
    ]

    def y_start(t, kind):
        ycopy(t, *mine[kind]).start()

    def y_wait(t, kind):
        ycopy(t, kind, arriving[kind], sib).wait_recv()

    def y_own(t):
        x_copies[t].wait()
        y_start(t, 0)
        y_start(t, 1)
        y_start(t, 3)

    def y_forward(t):
        y_wait(t, 0)
        y_start(t, 2)
        y_start(t, 4)
        y_wait(t, 1)
        y_start(t, 5)

    def y_relay(t):
        y_wait(t, 2)
        y_start(t, 6)

    def y_finish(t):
        half = xg.at[t, :, pl.ds(0, D // 2)]
        remote(half, half, ysend.at[0], yrecv.at[t, 3], sib).wait_recv()

    def project(t):
        rows = xg[t]
        part = jnp.dot(rows, wts[:, 0:512], preferred_element_type=F32)
        k0, k1 = part[:, 0:128], part[:, 128:256]
        for h in range(2):
            sbuf[h, t, 0] = jnp.concatenate(
                [k0[:, h * HD : (h + 1) * HD], k1[:, h * HD : (h + 1) * HD]], axis=1
            ).astype(BF16)
            value = part[:, 256 + h * 128 : 256 + (h + 1) * 128]
            sbuf[h, t, 1] = jnp.transpose(value).astype(BF16)
        if t == NT - 1:
            heads_start(t, 0)
        part = jnp.dot(rows, wts[:, 512:1024], preferred_element_type=F32)
        for m in range(2):
            turned = jnp.transpose(part[:, m * 128 : (m + 1) * 128] * SCALE).astype(BF16)
            for h in range(2):
                sq[h, t, m * HD : (m + 1) * HD, :] = turned[h * HD : (h + 1) * HD]
        pbuf[PAD + t * CH : PAD + (t + 1) * CH] = part[:, 256:512].astype(BF16)
        if t < NT - 1:
            heads_start(t, 0)
        heads_start(t, 1)

    def head_copies(t, h):
        device = (z * NX + 2 * c + h, y * 2 + x_core)
        pairs = [(sbuf.at[h, t], kv.at[0, 0, t, x_pos]), (sq.at[h, t], qin.at[t, x_pos])]
        far = [
            remote(src, dst, a2s.at[h, i], a2r.at[3 if i else t], device)
            for i, (src, dst) in enumerate(pairs)
        ]
        near = [
            pltpu.make_async_copy(src, dst, a2r.at[3 if i else t])
            for i, (src, dst) in enumerate(pairs)
        ]
        return 2 * c + h == x, far, near

    def heads_start(t, i):
        for h in range(2):
            to_self, far, near = head_copies(t, h)

            @pl.when(to_self)
            def _():
                near[i].start()

            @pl.when(jnp.logical_not(to_self))
            def _():
                far[i].start()

    def keys_wait(t):
        pltpu.make_async_copy(kv.at[1, 0, t], kv.at[0, 0, t], a2r.at[t]).wait()

    def queries_wait():
        pltpu.make_async_copy(qin, qin, a2r.at[3]).wait()

    def ring_copy(s, t):
        return remote(kv.at[0, s, t], kv.at[0, s + 1, t], rsend.at[0], rrecv.at[s + 1, t], ring_next)

    def sib_copy(s, t):
        return remote(kv.at[0, s, t], kv.at[1, s, t], ssend.at[0], srecv.at[s + jnp.where(s == NZ - 1, t // 2, 0)], sib)

    def sib_wait(s):
        remote(kv.at[0, s], kv.at[1, s], ssend.at[0], srecv.at[s], sib).wait_recv()

    def arrive_first(t):
        keys_wait(t)
        ring_copy(0, t).start()
        sib_copy(0, t).start()

    def arrive(s, t):
        remote(kv.at[0, s - 1, t], kv.at[0, s, t], rsend.at[0], rrecv.at[s, t], ring_next).wait_recv()

        @pl.when(s < NZ - 1)
        def _():
            ring_copy(s, t).start()

        sib_copy(s, t).start()

    def score(half, s, tile, slot, part, first):
        at = pl.ds(tile * TILE, TILE)
        keys = kv[half, s, part, :, 0].reshape(2 * CH, 128)
        scores = jnp.dot(keys, qt2[:, at], preferred_element_type=F32)
        sc[slot, part] = scores
        top = jnp.max(scores.reshape(2 * CH // 8, 8, TILE), axis=0)
        mx[slot] = top if first else jnp.maximum(mx[slot], top)

    def settle(tile, slot):
        at = pl.ds(tile * TILE, TILE)
        old = mrow[0:1, at]
        new = jnp.maximum(old, jnp.max(mx[slot], axis=0, keepdims=True))
        mrow[0:1, at] = new
        rescale = jnp.exp2(old - new)
        rs[slot, 0:1] = rescale
        lrow[:, at] = lrow[:, at] * rescale
        return new

    def weigh(tile, slot, part, new):
        at = pl.ds(tile * TILE, TILE)
        expo = jnp.exp2(sc[slot, part] - new)
        lrow[:, at] += jnp.sum(expo.reshape(2 * CH // 8, 8, TILE), axis=0)
        wt[slot, part] = expo.astype(BF16)

    def gather(half, s, tile, slot, parts):
        at = pl.ds(tile * TILE, TILE)
        values = jnp.concatenate(
            [kv[half, s, t, pos, 1] for t in parts for pos in range(2)], axis=1
        )
        weights = wt[slot, parts[0] : parts[-1] + 1].reshape(len(parts) * 2 * CH, TILE)
        acc[:, at] = acc[:, at] * rs[slot, 0:1] + jnp.dot(
            values, weights, preferred_element_type=F32
        )

    def attend(tasks, polls):
        for i in range(-1, len(tasks) + 1):
            if i in polls:
                polls[i]()
            ahead = tasks[i + 1] if i + 1 < len(tasks) else None
            here = tasks[i] if 0 <= i < len(tasks) else None
            behind = tasks[i - 1] if i >= 1 else None
            new = settle(here[2], i % 2) if here else None
            for part in range(NT):
                if ahead and part in ahead[3]:
                    score(*ahead[:3], (i + 1) % 2, part, part == ahead[3][0])
                if here and part in here[3]:
                    weigh(here[2], i % 2, part, new)
                if behind and part == behind[3][0]:
                    gather(*behind[:3], (i - 1) % 2, behind[3])

    def tasks_of(s, parts, some=None):
        return [(half, s, tile, parts) for half, tile in (both if some is None else some)]

    both = [(half, tile) for half in range(2) for tile in range(COLS // TILE)]

    for t in range(NT):
        y_own(t)
    remote(lamb.at[c], lamb.at[c], lms.at[0], lmr.at[0], sib).start()
    y_forward(0)
    y_forward(1)
    pltpu.make_async_copy(wts, wts, wsem.at[0]).wait()
    y_forward(2)
    y_relay(0)
    y_finish(0)
    project(0)
    y_relay(1)
    y_finish(1)
    y_relay(2)
    project(1)
    y_finish(2)
    project(2)
    arrive_first(0)
    arrive_first(1)

    up = remote(
        pbuf.at[pl.ds(TOK, PAD), :], pbuf.at[pl.ds(0, PAD), :], hs.at[0], hr.at[0],
        (lax.rem(me_sp + 1, NX * NZ), me_tp),
    )
    down = remote(
        pbuf.at[pl.ds(PAD, PAD), :], pbuf.at[pl.ds(PAD + TOK, PAD), :], hs.at[1], hr.at[1],
        (lax.rem(me_sp + NX * NZ - 1, NX * NZ), me_tp),
    )
    has_next, has_prev = me_sp < NX * NZ - 1, me_sp > 0

    @pl.when(has_next)
    def _():
        up.start()

    @pl.when(has_prev)
    def _():
        down.start()

    arrive_first(2)
    queries_wait()
    qt2[...] = jnp.zeros_like(qt2)
    for t in range(NT):
        for pos in range(2):
            at = 2 * pos * TOK + t * CH
            qt2[0:HD, at : at + CH] = qin[t, pos, 0:HD]
            qt2[HD : 2 * HD, TOK + at : TOK + at + CH] = qin[t, pos, HD : 2 * HD]

    pltpu.make_async_copy(wo.at[c], wo.at[c], wsem.at[1]).wait()

    def weight_copy(i):
        block = wo.at[c, lax.div(i, 4), pl.ds(pl.multiple_of(lax.rem(i, 4) * 64, 64), 64), :]
        return remote(block, block, wos.at[0], wor.at[0], sib)

    weight_copy(jnp.int32(0)).start()

    def pool():
        @pl.when(has_prev)
        def _():
            up.wait_recv()

        @pl.when(has_next)
        def _():
            down.wait_recv()

        pf[...] = pbuf[...].astype(F32)
        position = me_sp * TOK + lax.broadcasted_iota(jnp.int32, (TOK, 256), 0)
        total = NX * NZ * TOK
        result = jnp.zeros((TOK, 256), F32)
        for group in range(4):
            radius = 1 << group
            width = (408, 404, 400, 392)[group]
            if group == 0:
                ps[0, 0:width] = pf[0:width] + pf[1 : width + 1]
            else:
                ps[group, 0:width] = ps[group - 1, 0:width] + ps[group - 1, radius : width + radius]
            window = ps[group, PAD - radius : PAD - radius + TOK]
            low = jnp.maximum(position - radius, 0)
            high = jnp.minimum(position + radius, total)
            result = jnp.where(y == group, window / (high - low).astype(F32), result)
        pooled[...] = (result - pf[PAD : PAD + TOK]).astype(BF16)
        for owner in range(NY):
            for core in range(2):
                at = owner * 2 * OUT + core * OUT
                rows = pooled[at : at + OUT]

                @pl.when(c == core)
                def _():
                    pin[c, owner * OUT : (owner + 1) * OUT] = rows

                @pl.when(c != core)
                def _():
                    psib[owner * OUT : (owner + 1) * OUT] = rows

    pool_copy = remote(psib, pin.at[c], pxs.at[0], pxr.at[0], sib)

    def step(s, carry):
        weight_copy(s).start()
        def first():
            arrive(s, 0)
            sib_wait(s - 1)

        attend(tasks_of(s - 1, (0, 1, 2)), {4: first, 8: lambda: arrive(s, 1)})
        arrive(s, 2)
        return carry

    lax.fori_loop(1, NZ - 1, step, 0)
    weight_copy(jnp.int32(NZ - 1)).start()
    early, late = kv.at[0, NZ - 1, pl.ds(0, 2)], kv.at[0, NZ - 1, 2]

    def poll_first():
        arrive(NZ - 1, 0)
        sib_wait(NZ - 2)

    def poll_early():
        arrive(NZ - 1, 2)
        remote(early, early, ssend.at[0], srecv.at[NZ - 1], sib).wait_recv()

    def poll_late():
        remote(late, late, ssend.at[0], srecv.at[NZ], sib).wait_recv()

    by_pos = [both[3 * pos : 3 * pos + 3] + both[6 + 3 * pos : 9 + 3 * pos] for pos in range(2)]
    attend(
        tasks_of(NZ - 2, (0, 1, 2)) + tasks_of(NZ - 1, (0, 1)) + tasks_of(NZ - 1, (2,), by_pos[0]),
        {4: poll_first, 8: lambda: arrive(NZ - 1, 1), 17: poll_early, 23: poll_late},
    )

    remote(lamb.at[1 - c], lamb.at[1 - c], lms.at[0], lmr.at[0], sib).wait_recv()
    lam = jnp.sum(
        jnp.where(lane == x_pos, lamb[x_core], 0.0)[0:1], axis=1, keepdims=True
    )
    gain = gain_ref[...]
    row8 = lax.broadcasted_iota(jnp.int32, (8, TOK), 0)
    def back_copies(pos, core):
        if core is None:
            src, dst, send, recv = lgs.at[pos], lg_in.at[x_pos], ls.at[pos], lr.at[0]
            device = (z * NX + 2 * c + pos, y * 2 + x_core)
            to_self = 2 * c + pos == x
        else:
            src, dst, send, recv = ob.at[pos, core], at_in.at[x], bs.at[pos, core], br.at[0]
            device = (z * NX + 2 * c + pos, y * 2 + core)
            to_self = jnp.logical_and(2 * c + pos == x, c == core)
        return to_self, remote(src, dst, send, recv, device), pltpu.make_async_copy(src, dst, recv)

    back = [(pos, core) for core in (0, 1, None) for pos in range(2)]
    for pos in range(2):
        if pos == 1:
            attend(tasks_of(NZ - 1, (2,), by_pos[1]), {})
        a0, a1 = pl.ds(2 * pos * TOK, TOK), pl.ds((2 * pos + 1) * TOK, TOK)
        l0 = jnp.sum(lrow[:, a0], axis=0, keepdims=True)
        l1 = jnp.sum(lrow[:, a1], axis=0, keepdims=True)
        diff = acc[:, a0] * (1.0 / l0) - acc[:, a1] * (lam / l1)
        mean = jnp.sum(diff * diff, axis=0, keepdims=True) * (1.0 / 128.0)
        normed = jnp.transpose(diff * lax.rsqrt(mean + 1e-05))
        rows = (normed * gain).astype(BF16)
        for owner in range(NY):
            for core in range(2):
                at = owner * 2 * OUT + core * OUT
                ob[pos, core, owner * OUT : (owner + 1) * OUT] = rows[at : at + OUT]
        log0 = (mrow[0:1, a0] + jnp.log2(l0)) * LN2
        log1 = (mrow[0:1, a1] + jnp.log2(l1)) * LN2
        lgs[pos] = jnp.where(row8 == 0, log0, log1)
        for core in (0, 1, None):
            to_self, far, near = back_copies(pos, core)

            @pl.when(to_self)
            def _():
                near.start()

            @pl.when(jnp.logical_not(to_self))
            def _():
                far.start()

    yp, ym = (me_sp, lax.rem(y + 1, NY) * 2 + c), (me_sp, lax.rem(y + NY - 1, NY) * 2 + c)
    pool()
    pool_copy.start()
    remote(psib, pin.at[1 - c], pxs.at[0], pxr.at[0], sib).wait_recv()
    remote(wo.at[1 - c], wo.at[1 - c], wos.at[0], wor.at[0], sib).wait_recv()
    pltpu.make_async_copy(at_in, at_in, br.at[0]).wait()
    for r in range(NY):
        rows = pl.ds(pl.multiple_of(lax.rem(y + r, NY) * OUT, 16), OUT)
        for h in range(NX):
            at = (h // 2) * 512 + (h % 2) * 128
            amat[r * OUT : (r + 1) * OUT, at : at + 128] = at_in[h, rows, :]
        for core in range(2):
            at = core * 512 + 256
            amat[r * OUT : (r + 1) * OUT, at : at + 256] = pin[core, rows, :]

    def via_copy(j, e):
        return remote(via_s.at[j], via_r.at[j], vs.at[0], vr.at[j], yp if e == 0 else ym)

    def fin_copy(src, way, j):
        return remote(src, fin.at[way, j], fs.at[0], fr.at[j], yp if way == 0 else ym)

    def out_step(jj, carry):
        for e in range(2):
            j = jj * 2 + e
            at = pl.ds(pl.multiple_of(j * NB, NB), NB)
            weights = wo[:, :, :, at].reshape(1024, NB)
            part = jnp.dot(amat[...], weights, preferred_element_type=F32)
            via_s[j] = part[2 * OUT : 3 * OUT].astype(BF16)
            via_copy(j, e).start()
            up_rows, down_rows = part[OUT : 2 * OUT], part[3 * OUT :]
            raw_s[j] = (down_rows if e == 0 else up_rows).astype(BF16)
            fin_copy(raw_s.at[j], 1 - e, j).start()
            keep[j] = up_rows if e == 0 else down_rows
            own[:, at] = part[0:OUT]
        return carry

    lax.fori_loop(0, D // NB // 2, out_step, 0)

    def pass_step(jj, carry):
        for e in range(2):
            j = jj * 2 + e
            via_copy(j, e).wait_recv()
            sum_s[j] = (keep[j] + via_r[j].astype(F32)).astype(BF16)
            fin_copy(sum_s.at[j], e, j).start()
        return carry

    lax.fori_loop(0, D // NB // 2, pass_step, 0)

    pltpu.make_async_copy(lg_in, lg_in, lr.at[0]).wait()
    for hh in range(2):
        logt_ref[0, hh : hh + 1] = lg_in[hh, 0:1]
        logt_ref[1, hh : hh + 1] = lg_in[hh, 1:2]
    def last_step(j, carry):
        at = pl.ds(pl.multiple_of(j * NB, NB), NB)
        pltpu.make_async_copy(fin.at[:, j], fin.at[:, j], fr.at[j]).wait()
        mixed_ref[:, at] = (
            own[:, at] + fin[0, j].astype(F32) + fin[1, j].astype(F32)
        ).astype(BF16)
        return carry

    lax.fori_loop(0, D // NB, last_step, 0)

    sent = xg.at[:, :, pl.ds(0, 7 * FEAT)]
    remote(sent, sent, ysend.at[0], yrecv.at[0, 0], sib).wait_send()
    for h in range(2):
        @pl.when(2 * c + h != x)
        def _():
            remote(sbuf.at[h], sbuf.at[h], a2s.at[h, 0], a2r.at[0], sib).wait_send()
            remote(sq.at[h], sq.at[h], a2s.at[h, 1], a2r.at[3], sib).wait_send()

    ring_sent = kv.at[0, pl.ds(0, NZ - 1)]
    remote(ring_sent, ring_sent, rsend.at[0], rrecv.at[1, 0], ring_next).wait_send()
    remote(kv.at[0], kv.at[0], ssend.at[0], srecv.at[0], sib).wait_send()
    remote(wo.at[c], wo.at[c], wos.at[0], wor.at[0], sib).wait_send()
    remote(via_s, via_s, vs.at[0], vr.at[0], yp).wait_send()
    remote(fin, fin, fs.at[0], fr.at[0], yp).wait_send()
    remote(lamb.at[c], lamb.at[c], lms.at[0], lmr.at[0], sib).wait_send()
    pool_copy.wait_send()

    @pl.when(has_next)
    def _():
        up.wait_send()

    @pl.when(has_prev)
    def _():
        down.wait_send()

    for pos, core in back:
        to_self, far, near = back_copies(pos, core)

        @pl.when(jnp.logical_not(to_self))
        def _():
            far.wait_send()


def on_device(inputs, qw, kw, vw, pw, lam, gain, ow, pow_):
    any_ = pl.BlockSpec(memory_space=pltpu.HBM)
    vmem = pl.BlockSpec(memory_space=pltpu.VMEM)
    smem = pl.BlockSpec(memory_space=pltpu.SMEM)
    dma = pltpu.SemaphoreType.DMA
    scratch = [
        pltpu.VMEM((NT, CH, D), BF16),
        pltpu.VMEM((D, 1024), BF16),
        pltpu.VMEM((2, 2, 256, D), BF16),
        pltpu.VMEM((2, NT, 2, 128, 128), BF16),
        pltpu.VMEM((2, NT, 128, 128), BF16),
        pltpu.VMEM((2, NZ, NT, 2, 2, 128, 128), BF16),
        pltpu.VMEM((NT, 2, 128, 128), BF16),
        pltpu.VMEM((128, COLS), BF16),
        pltpu.VMEM((128, COLS), F32),
        pltpu.VMEM((8, COLS), F32),
        pltpu.VMEM((8, COLS), F32),
        pltpu.VMEM((2, 8, 128), F32),
        pltpu.VMEM((TOK + 2 * PAD, 256), BF16),
        pltpu.VMEM((TOK + 2 * PAD, 256), F32),
        pltpu.VMEM((4, TOK + 2 * PAD, 256), F32),
        pltpu.VMEM((TOK, 256), BF16),
        pltpu.VMEM((2, 192, 256), BF16),
        pltpu.VMEM((192, 256), BF16),
        pltpu.VMEM((2, 2, 192, 128), BF16),
        pltpu.VMEM((4, 192, 128), BF16),
        pltpu.VMEM((2, 8, TOK), F32),
        pltpu.VMEM((2, 8, TOK), F32),
        pltpu.VMEM((192, 1024), BF16),
        pltpu.VMEM((OUT, D), F32),
        pltpu.VMEM((8, OUT, NB), F32),
        pltpu.VMEM((8, OUT, NB), BF16),
        pltpu.VMEM((8, OUT, NB), BF16),
        pltpu.VMEM((8, OUT, NB), BF16),
        pltpu.VMEM((8, OUT, NB), BF16),
        pltpu.VMEM((2, 8, OUT, NB), BF16),
        pltpu.VMEM((2, NT, 2 * CH, TILE), F32),
        pltpu.VMEM((2, 8, TILE), F32),
        pltpu.VMEM((2, 8, TILE), F32),
        pltpu.VMEM((2, NT, 2 * CH, TILE), BF16),
        dma((NT,)), dma((2,)), dma((1,)), dma((NT, 4)),
        dma((2, 2)), dma((4,)),
        dma((1,)), dma((NZ, NT)), dma((1,)), dma((NZ + 1,)),
        dma((1,)), dma((1,)), dma((1,)), dma((1,)), dma((2,)), dma((2,)),
        dma((1,)), dma((1,)), dma((2, 2)), dma((1,)), dma((2,)), dma((1,)),
        dma((1,)), dma((8,)), dma((1,)), dma((8,)),
    ]
    return pl.pallas_call(
        kernel,
        out_shape=(
            jax.ShapeDtypeStruct((OUT, D), BF16),
            jax.ShapeDtypeStruct((2, 2, TOK), F32),
        ),
        in_specs=[smem, vmem] + [any_] * 7,
        out_specs=(vmem, vmem),
        scratch_shapes=scratch,
        compiler_params=pltpu.CompilerParams(
            collective_id=0, has_side_effects=True, vmem_limit_bytes=54700 * 1024
        ),
    )(lam, gain.reshape(1, 128), inputs, qw, kw, vw, pw, ow, pow_)


def solution(mesh):
    in_specs = (
        P("sp", "tp"),
        P(None, None, "tp"),
        P(None, None, "tp"),
        P(None, "tp"),
        P(None, "tp"),
        P("tp"),
        P(),
        P("tp", None),
        P("tp", None),
    )
    out_specs = (P(("sp", "tp"), None), P(None, "tp", "sp"))
    return jax.shard_map(
        on_device, mesh=mesh, in_specs=in_specs, out_specs=out_specs, check_vma=False
    )
```
